32 devices in a mesh: rep: 4 (over z), fs: 4 (over y, x), tp: 2 (over core).
Axes of the slice: x: 2, y: 2, z: 4, core: 2. Of those that a mesh axis runs over, the one named last changes fastest.
Arguments:
- skip_stream_entry: bfloat16 [4096, 2048], P(('rep', 'fs')), may hold values from -6 to 6
- sequence_blender_factor: float32 [2048], replicated, may hold values from 0.1 to 1.9
- product_projector: float32 [2048, 1024], P('fs', 'tp'), may hold values from -0.125 to 0.125
- product_side_factors: float32 [1024], P('tp'), may hold values from 0.3 to 3
- placewise_projector: float32 [2048, 1024], P('fs', 'tp'), may hold values from -0.125 to 0.125
- placewise_entry_factors: float32 [1024], P('tp'), may hold values from 0.7 to 11.2, as said below
- placewise_rescale_factor: float32 [1024], P('tp'), may hold values from 0.1 to 1.9
- place_cluster_operator: bfloat16 [8, 128, 128], replicated, may hold values from -0.5 to 0.5
- placewise_offset_vector: float32 [8, 128], replicated, may hold values from 0.1 to 1.9
- blender_result_projector: float32 [1024, 2048], P('tp', 'fs'), may hold values from -0.1875 to 0.1875
- blender_result_factors: float32 [2048], P('fs'), may hold values from 0.3 to 3
- feedforward_norm_factor: float32 [2048], replicated, may hold values from 0.1 to 1.9
- switch_projector: float32 [2048, 2816], P('fs', 'tp'), may hold values from -0.125 to 0.125
- switch_factors: float32 [2816], P('tp'), may hold values from 0.3 to 3
- expand_projector: float32 [2048, 2816], P('fs', 'tp'), may hold values from -0.125 to 0.125
- expand_factors: float32 [2816], P('tp'), may hold values from 0.3 to 3
- contract_projector: float32 [2816, 2048], P('tp', 'fs'), may hold values from -0.109375 to 0.109375
- contract_factors: float32 [2048], P('fs'), may hold values from 0.3 to 3
Outputs:
- result: bfloat16 [4096, 2048], P(('rep', 'fs'), 'tp')
The draws below stay inside these ranges and needn't reach their ends.
Inputs may be any that keep to these rules, and one draw needn't show every extreme that they name: `placewise_entry_factors`: positive column scales.
All inputs are finite; a program needn't handle non-finite values.
Results may differ from the reference program's by a relative error of at most 0.023.
Values may be sent and summed in bfloat16 or wider, within the bound.
No kernel may reach another device: no remote copies, remote signals or barrier semaphores. Data moves between devices by JAX's collectives and lax.ppermute only.
A program may use at most 64 MiB of HBM per device.

```python
import math
import jax
import jax.numpy as jnp
from jax import lax

EMBED_DIMENSION = 2048
BLENDER_FEATURES = 1024
GROUP_DIM = 128
BLOCK = 128
FF = 2816
SHARED_SEQ_STEPS = 256
GROUPS = 8
TOKENS = 4096
N_REP = 4
N_FS = 4
N_TP = 2


def draw_placewise_entry_factors(key, part):
    column_pos = jnp.arange(BLENDER_FEATURES, dtype=jnp.float32) / (BLENDER_FEATURES - 1)
    rising = jnp.exp(jnp.log(4.0) * column_pos)
    rough_part = jnp.exp(jax.random.uniform(key, (BLENDER_FEATURES,), jnp.float32, jnp.log(0.7), jnp.log(1.4)))
    return rising * rough_part


def levels(stream_key, extent, cuts, least, largest):
    level, own = 1.0, jax.random.fold_in(stream_key, 6)
    for position, shards_of in cuts:
        heights = jnp.exp(jax.random.uniform(jax.random.fold_in(own, position), (shards_of,), jnp.float32, least / len(cuts), largest / len(cuts)))
        level = level * jnp.repeat(heights, extent[position] // shards_of).reshape([-1 if axis == position else 1 for axis in range(len(extent))])
    return level


def bell_draw(rng, dims, scale, reach, split=(), kind=jnp.bfloat16):
    drawn = jax.random.normal(rng, dims, jnp.float32) * scale
    if len(split) > 0:
        drawn = levels(rng, dims, split, -0.22, 0.18) * drawn
    return jnp.clip(drawn, min=-reach, max=reach).astype(kind)


def setup_inputs(seed: int = 0) -> dict:
    key_of = jax.random.split(jax.random.key(seed), 19)
    skip_stream_entry = bell_draw(key_of[0], (TOKENS, EMBED_DIMENSION), 1.0, 6.0, ((0, 16),))
    sequence_blender_factor = jnp.clip(1.0 + 0.18 * jax.random.normal(key_of[1], (EMBED_DIMENSION,), jnp.float32), 0.1, 1.9)
    product_projector = bell_draw(key_of[2], (EMBED_DIMENSION, BLENDER_FEATURES), EMBED_DIMENSION ** -0.5, 0.125, ((0, 4), (1, 2)), jnp.float32)
    product_side_factors = jnp.clip(jnp.exp(math.log(3.0) - 2.3025851 * jax.random.uniform(key_of[3], (BLENDER_FEATURES,), jnp.float32) ** levels(key_of[3], (BLENDER_FEATURES,), ((0, 2),), -0.2, 0.2)), 0.3, 3.0)
    placewise_projector = bell_draw(key_of[4], (EMBED_DIMENSION, BLENDER_FEATURES), EMBED_DIMENSION ** -0.5, 0.125, ((0, 4), (1, 2)), jnp.float32)
    placewise_entry_factors = draw_placewise_entry_factors(jax.random.fold_in(key_of[18], 71), 0)
    placewise_rescale_factor = jnp.clip(1.0 + 0.18 * jax.random.normal(key_of[6], (BLENDER_FEATURES,), jnp.float32), 0.1, 1.9)
    place_cluster_operator = bell_draw(key_of[7], (GROUPS, BLOCK, BLOCK), BLOCK ** -0.5, 0.5)
    placewise_offset_vector = jnp.clip(1.0 + 0.18 * jax.random.normal(key_of[8], (GROUPS, BLOCK), jnp.float32), 0.1, 1.9)
    blender_result_projector = bell_draw(key_of[9], (BLENDER_FEATURES, EMBED_DIMENSION), BLENDER_FEATURES ** -0.5, 0.1875, ((0, 2), (1, 4)), jnp.float32)
    blender_result_factors = jnp.clip(jnp.exp(math.log(3.0) - 2.3025851 * jax.random.uniform(key_of[10], (EMBED_DIMENSION,), jnp.float32) ** levels(key_of[10], (EMBED_DIMENSION,), ((0, 4),), -0.2, 0.2)), 0.3, 3.0)
    feedforward_norm_factor = jnp.clip(1.0 + 0.18 * jax.random.normal(key_of[11], (EMBED_DIMENSION,), jnp.float32), 0.1, 1.9)
    switch_projector = bell_draw(key_of[12], (EMBED_DIMENSION, FF), EMBED_DIMENSION ** -0.5, 0.125, ((0, 4), (1, 2)), jnp.float32)
    switch_factors = jnp.clip(jnp.exp(math.log(3.0) - 2.3025851 * jax.random.uniform(key_of[13], (FF,), jnp.float32) ** levels(key_of[13], (FF,), ((0, 2),), -0.2, 0.2)), 0.3, 3.0)
    expand_projector = bell_draw(key_of[14], (EMBED_DIMENSION, FF), EMBED_DIMENSION ** -0.5, 0.125, ((0, 4), (1, 2)), jnp.float32)
    expand_factors = jnp.clip(jnp.exp(math.log(3.0) - 2.3025851 * jax.random.uniform(key_of[15], (FF,), jnp.float32) ** levels(key_of[15], (FF,), ((0, 2),), -0.2, 0.2)), 0.3, 3.0)
    contract_projector = bell_draw(key_of[16], (FF, EMBED_DIMENSION), FF ** -0.5, 0.109375, ((0, 2), (1, 4)), jnp.float32)
    contract_factors = jnp.clip(jnp.exp(math.log(3.0) - 2.3025851 * jax.random.uniform(key_of[17], (EMBED_DIMENSION,), jnp.float32) ** levels(key_of[17], (EMBED_DIMENSION,), ((0, 4),), -0.2, 0.2)), 0.3, 3.0)
    return dict(skip_stream_entry=skip_stream_entry, sequence_blender_factor=sequence_blender_factor, product_projector=product_projector, product_side_factors=product_side_factors, placewise_projector=placewise_projector, placewise_entry_factors=placewise_entry_factors, placewise_rescale_factor=placewise_rescale_factor, place_cluster_operator=place_cluster_operator, placewise_offset_vector=placewise_offset_vector, blender_result_projector=blender_result_projector, blender_result_factors=blender_result_factors, feedforward_norm_factor=feedforward_norm_factor, switch_projector=switch_projector, switch_factors=switch_factors, expand_projector=expand_projector, expand_factors=expand_factors, contract_projector=contract_projector, contract_factors=contract_factors)


epsilon = 1e-06

def normalize(values, gain):
    return values * lax.rsqrt(lax.optimization_barrier(jnp.mean(values * values, axis=-1, keepdims=True)) + epsilon) * gain

def shard_total(activations, weight, scale):
    shards = activations.astype(jnp.float32).reshape(activations.shape[0], N_TP, -1)
    pieces = weight.astype(jnp.float32).reshape(N_TP, -1, weight.shape[1])
    partial_value = jnp.einsum('tkc,kcd->ktd', shards, pieces) * scale
    rounded = lax.optimization_barrier(partial_value.astype(jnp.bfloat16))
    return lax.optimization_barrier(jnp.sum(rounded.astype(jnp.float32), axis=0))

def reference(skip_stream_entry, sequence_blender_factor, product_projector, product_side_factors, placewise_projector, placewise_entry_factors, placewise_rescale_factor, place_cluster_operator, placewise_offset_vector, blender_result_projector, blender_result_factors, feedforward_norm_factor, switch_projector, switch_factors, expand_projector, expand_factors, contract_projector, contract_factors):
    product_lowered = product_projector.astype(jnp.bfloat16)
    spread_low = placewise_projector.astype(jnp.bfloat16)
    mix_out_low = blender_result_projector.astype(jnp.bfloat16)
    gate_low = switch_projector.astype(jnp.bfloat16)
    up_low = expand_projector.astype(jnp.bfloat16)
    down_low = contract_projector.astype(jnp.bfloat16)
    causal = jnp.tril(jnp.ones((BLOCK, BLOCK), dtype=bool))
    masked = jnp.where(causal[None], place_cluster_operator, jnp.zeros_like(place_cluster_operator)).astype(jnp.float32)

    def layer(rows):
        standardized_stream = normalize(rows.astype(jnp.float32), sequence_blender_factor).astype(jnp.bfloat16)
        product_portion = jax.nn.gelu(jnp.dot(standardized_stream, product_lowered, preferred_element_type=jnp.float32) * product_side_factors)
        spread = jax.nn.gelu(jnp.dot(standardized_stream, spread_low, preferred_element_type=jnp.float32) * placewise_entry_factors)
        spread_normed = normalize(spread, placewise_rescale_factor).astype(jnp.bfloat16)
        blocks = spread_normed.astype(jnp.float32).reshape(SHARED_SEQ_STEPS // BLOCK, BLOCK, GROUPS, GROUP_DIM)
        blended_sequence = jnp.einsum('gts,nsgc->ntgc', masked, blocks, precision=lax.Precision.HIGHEST)
        blended_sequence = blended_sequence + placewise_offset_vector.T[None, :, :, None]
        switched_inner = (product_portion * blended_sequence.reshape(SHARED_SEQ_STEPS, BLENDER_FEATURES)).astype(jnp.bfloat16)
        stream = (rows.astype(jnp.float32) + shard_total(switched_inner, mix_out_low, blender_result_factors)).astype(jnp.bfloat16)
        ffn_normed = normalize(stream.astype(jnp.float32), feedforward_norm_factor).astype(jnp.bfloat16)
        gate = jnp.dot(ffn_normed, gate_low, preferred_element_type=jnp.float32) * switch_factors
        upper = jnp.dot(ffn_normed, up_low, preferred_element_type=jnp.float32) * expand_factors
        active = (jax.nn.silu(gate) * upper).astype(jnp.bfloat16)
        return (stream.astype(jnp.float32) + shard_total(active, down_low, contract_factors)).astype(jnp.bfloat16)
    grouped = skip_stream_entry.reshape(N_REP * N_FS, SHARED_SEQ_STEPS, EMBED_DIMENSION)
    return lax.map(layer, grouped).reshape(TOKENS, EMBED_DIMENSION)
```

```python
import jax
import jax.numpy as jnp
from jax import lax
from jax.sharding import PartitionSpec as P

BLENDER_FEATURES = 1024
GROUP_DIM = 128
BLOCK = 128


epsilon = 1e-06


def normalize(values, gain):
    return values * lax.rsqrt(jnp.mean(values * values, axis=-1, keepdims=True) + epsilon) * gain


def assembled_entries(pieces, activations):
    segments = (
        lax.all_gather(pieces[0], "fs", axis=0, tiled=True),
        lax.all_gather(pieces[1], "fs", axis=0, tiled=True),
    )
    return tuple(
        (jnp.dot(activations, segment, preferred_element_type=jnp.float32) for segment in segments)
    )


def collect_cols(shard_rows, activations, scales):
    return (
        jnp.dot(
            activations,
            lax.all_gather(shard_rows, "fs", axis=1, tiled=True),
            preferred_element_type=jnp.float32,
        )
        * scales
    )


def on_device_gathered(
    skip_stream_entry,
    sequence_blender_factor,
    product_projector,
    product_side_factors,
    placewise_projector,
    placewise_entry_factors,
    placewise_rescale_factor,
    place_cluster_operator,
    placewise_offset_vector,
    blender_result_projector,
    blender_result_factors,
    feedforward_norm_factor,
    switch_projector,
    switch_factors,
    expand_projector,
    expand_factors,
    contract_projector,
    contract_factors,
):
    device_sequence_steps = skip_stream_entry.shape[0]
    tp_index = lax.axis_index("tp")
    own_features = skip_stream_entry.shape[1] // lax.axis_size("tp")
    out_scales = (
        lax.all_gather(blender_result_factors, "fs", axis=0, tiled=True),
        lax.all_gather(contract_factors, "fs", axis=0, tiled=True),
    )
    standardized_stream = normalize(
        skip_stream_entry.astype(jnp.float32), sequence_blender_factor
    ).astype(jnp.bfloat16)
    product_plain, diffuse_plain = assembled_entries(
        (product_projector.astype(jnp.bfloat16), placewise_projector.astype(jnp.bfloat16)),
        standardized_stream,
    )
    product_portion = jax.nn.gelu(product_plain * product_side_factors)
    spread = jax.nn.gelu(diffuse_plain * placewise_entry_factors)
    feature_total = spread.shape[1]
    squares = lax.psum(jnp.sum(spread * spread, axis=1), "tp")
    factor = lax.rsqrt(squares / BLENDER_FEATURES + epsilon)
    spread_normed = (spread * factor[:, None] * placewise_rescale_factor).astype(jnp.bfloat16)
    group_span = min(feature_total, GROUP_DIM)
    group_count = max(1, feature_total // GROUP_DIM)
    first_group = tp_index * feature_total // GROUP_DIM
    causal = jnp.tril(jnp.ones((BLOCK, BLOCK), dtype=bool))
    local_weight = lax.dynamic_slice_in_dim(place_cluster_operator, first_group, group_count, 0)
    local_weight = jnp.where(causal[None], local_weight, jnp.zeros_like(local_weight))
    local_bias = lax.dynamic_slice_in_dim(placewise_offset_vector, first_group, group_count, 0)
    blocks = spread_normed.reshape(device_sequence_steps // BLOCK, BLOCK, group_count, group_span)
    blended_sequence = jnp.einsum(
        "gts,nsgc->ntgc", local_weight, blocks, preferred_element_type=jnp.float32
    )
    blended_sequence = blended_sequence + local_bias.T[None, :, :, None]
    switched_inner = (
        product_portion * blended_sequence.reshape(device_sequence_steps, feature_total)
    ).astype(jnp.bfloat16)
    mix_terms = collect_cols(
        blender_result_projector.astype(jnp.bfloat16), switched_inner, out_scales[0]
    )
    mix_total = lax.psum_scatter(
        mix_terms.astype(jnp.bfloat16), "tp", scatter_dimension=1, tiled=True
    ).astype(jnp.float32)
    own_input = lax.dynamic_slice_in_dim(
        skip_stream_entry, tp_index * own_features, own_features, 1
    )
    stream = (own_input.astype(jnp.float32) + mix_total).astype(jnp.bfloat16)
    stream_whole = lax.all_gather(stream, "tp", axis=1, tiled=True)
    ffn_normed = normalize(stream_whole.astype(jnp.float32), feedforward_norm_factor).astype(
        jnp.bfloat16
    )
    gate_raw, up_raw = assembled_entries(
        (switch_projector.astype(jnp.bfloat16), expand_projector.astype(jnp.bfloat16)), ffn_normed
    )
    active = (jax.nn.silu(gate_raw * switch_factors) * (up_raw * expand_factors)).astype(
        jnp.bfloat16
    )
    ffn_terms = collect_cols(contract_projector.astype(jnp.bfloat16), active, out_scales[1])
    ffn_total = lax.psum_scatter(
        ffn_terms.astype(jnp.bfloat16), "tp", scatter_dimension=1, tiled=True
    ).astype(jnp.float32)
    return (stream.astype(jnp.float32) + ffn_total).astype(jnp.bfloat16)


def half_of(array, index, axis):
    lower, upper = jnp.split(array, 2, axis=axis)
    return jnp.where(index == 0, lower, upper)


def swap_pairs(size, bit):
    return [(i, i ^ bit) for i in range(size)]


def gather_first(own):
    size = lax.axis_size("fs")
    return (
        lax.ppermute(own, "fs", swap_pairs(size, 1)),
        lax.ppermute(own, "fs", swap_pairs(size, 2)),
    )


def gather_second(from_one, from_two, axis):
    size = lax.axis_size("fs")
    lower = jnp.split(from_two, 2, axis=axis)[0]
    upper = jnp.split(from_one, 2, axis=axis)[1]
    return (
        lax.ppermute(lower, "fs", swap_pairs(size, 1)),
        lax.ppermute(upper, "fs", swap_pairs(size, 2)),
    )


def dot32(a, b):
    return jnp.dot(a, b, preferred_element_type=jnp.float32)


def entry_product(blocks, own, one, two, far):
    cut = far[0].shape[0]
    total = dot32(blocks[0], own) + dot32(blocks[1], one) + dot32(blocks[2], two)
    return total + dot32(blocks[3][:, :cut], far[0]) + dot32(blocks[3][:, cut:], far[1])


def on_device_paired(
    skip_stream_entry,
    sequence_blender_factor,
    product_projector,
    product_side_factors,
    placewise_projector,
    placewise_entry_factors,
    placewise_rescale_factor,
    place_cluster_operator,
    placewise_offset_vector,
    blender_result_projector,
    blender_result_factors,
    feedforward_norm_factor,
    switch_projector,
    switch_factors,
    expand_projector,
    expand_factors,
    contract_projector,
    contract_factors,
):
    bf16, f32 = jnp.bfloat16, jnp.float32
    steps, width = skip_stream_entry.shape
    rep_size, fs_size, tp_size = (lax.axis_size(a) for a in ("rep", "fs", "tp"))
    tp_index = lax.axis_index("tp")
    fs_index = lax.axis_index("fs")
    side = lax.axis_index("rep") % 2
    band = width // fs_size
    upper_band = fs_index // 2

    def across_tp(a):
        return lax.ppermute(a, "tp", swap_pairs(tp_size, 1))

    def across_rep(a):
        return lax.ppermute(a, "rep", swap_pairs(rep_size, 1))

    def across_both(a):
        pairs = [
            (r * tp_size + t, (r ^ 1) * tp_size + (t ^ 1))
            for r in range(rep_size)
            for t in range(tp_size)
        ]
        return lax.ppermute(a, ("rep", "tp"), pairs)

    def bands_of(array):
        return [
            lax.dynamic_slice_in_dim(array, (fs_index ^ k) * band, band, 1)
            for k in range(fs_size)
        ]

    def gains_of(gain):
        return [
            lax.dynamic_slice_in_dim(gain, (fs_index ^ k) * band, band, 0)
            for k in range(fs_size)
        ]

    sent = across_rep(half_of(skip_stream_entry, tp_index, 1))
    other = across_tp(sent)

    in_own = jnp.concatenate(
        [half_of(product_projector, side, 1), half_of(placewise_projector, side, 1)], axis=1
    ).astype(bf16)
    out_own = half_of(blender_result_projector, side, 0).astype(bf16)
    in_one, in_two = gather_first(in_own)
    out_one, out_two = gather_first(out_own)
    scales_own = jnp.stack([blender_result_factors, contract_factors])
    scales = [scales_own] + [
        lax.ppermute(scales_own, "fs", swap_pairs(fs_size, k)) for k in range(1, fs_size)
    ]
    in_far = gather_second(in_one, in_two, 0)
    out_far = gather_second(out_one, out_two, 1)
    ffn_own = jnp.concatenate(
        [half_of(switch_projector, side, 1), half_of(expand_projector, side, 1)], axis=1
    ).astype(bf16)
    down_own = half_of(contract_projector, side, 0).astype(bf16)
    ffn_own, in_far = lax.optimization_barrier((ffn_own, in_far))
    ffn_one, ffn_two = gather_first(ffn_own)
    down_own, out_far = lax.optimization_barrier((down_own, out_far))
    down_one, down_two = gather_first(down_own)
    ffn_far = gather_second(ffn_one, ffn_two, 0)
    down_far = gather_second(down_one, down_two, 1)

    partner_rows = jnp.where(
        tp_index == 0,
        jnp.concatenate([sent, other], axis=1),
        jnp.concatenate([other, sent], axis=1),
    )
    rows = jnp.concatenate([skip_stream_entry, partner_rows], axis=0)
    row_bands = bands_of(rows)

    def normed_bands(bands, gain):
        wide = [b.astype(f32) for b in bands]
        total = sum(jnp.sum(b * b, axis=-1, keepdims=True) for b in wide)
        factor = lax.rsqrt(total / width + epsilon)
        return [(b * factor * g).astype(bf16) for b, g in zip(wide, gains_of(gain))]

    normed = normed_bands(row_bands, sequence_blender_factor)
    entry = entry_product(normed, in_own, in_one, in_two, in_far)
    channels = entry.shape[1] // 2
    carrier = jax.nn.gelu(entry[:, :channels] * half_of(product_side_factors, side, 0))
    spread = jax.nn.gelu(entry[:, channels:] * half_of(placewise_entry_factors, side, 0))
    squares = jnp.sum(spread * spread, axis=1)
    turned = jnp.concatenate([squares[steps:], squares[:steps]])
    squares = (squares + across_tp(squares)) + (across_rep(turned) + across_both(turned))
    factor = lax.rsqrt(squares / BLENDER_FEATURES + epsilon)
    spread_normed = (
        spread * factor[:, None] * half_of(placewise_rescale_factor, side, 0)
    ).astype(bf16)
    group_count = channels // GROUP_DIM
    first_group = (tp_index * 2 + side) * group_count
    causal = jnp.tril(jnp.ones((BLOCK, BLOCK), dtype=bool))
    local_weight = lax.dynamic_slice_in_dim(place_cluster_operator, first_group, group_count, 0)
    local_weight = jnp.where(causal[None], local_weight, jnp.zeros_like(local_weight))
    local_bias = lax.dynamic_slice_in_dim(placewise_offset_vector, first_group, group_count, 0)
    blocks = spread_normed.reshape(2 * steps // BLOCK, BLOCK, group_count, GROUP_DIM)
    blended = jnp.einsum("gts,nsgc->ntgc", local_weight, blocks, preferred_element_type=f32)
    blended = blended + local_bias.T[None, :, :, None]
    gated = (carrier * blended.reshape(2 * steps, channels)).astype(bf16)

    def result_bands(act, own, one, two, far, which):
        pieces = (own, one, two, jnp.concatenate(far, axis=1))
        return [
            (dot32(act, w) * s[which]).astype(bf16) for w, s in zip(pieces, scales)
        ]

    keep_low = tp_index == upper_band

    def tp_reduced(low, high):
        mine = jnp.where(keep_low, low, high)
        theirs = jnp.where(keep_low, high, low)
        return mine.astype(f32) + across_tp(theirs).astype(f32)

    parts = result_bands(gated, out_own, out_one, out_two, out_far, 0)
    mixed = tp_reduced(
        jnp.concatenate(parts[:2], axis=1), jnp.concatenate(parts[2:], axis=1)
    ).astype(bf16)
    mixed_total = mixed.astype(f32) + across_rep(
        jnp.concatenate([mixed[steps:], mixed[:steps]], axis=0)
    ).astype(f32)
    low_rows = jnp.concatenate(row_bands[:2], axis=1)
    high_rows = jnp.concatenate(row_bands[2:], axis=1)
    stream = (jnp.where(keep_low, low_rows, high_rows).astype(f32) + mixed_total).astype(bf16)
    stream_other = across_tp(stream)
    low_stream = jnp.where(keep_low, stream, stream_other)
    high_stream = jnp.where(keep_low, stream_other, stream)
    stream_bands = [
        low_stream[:, :band],
        low_stream[:, band:],
        high_stream[:, :band],
        high_stream[:, band:],
    ]
    ffn_normed = normed_bands(stream_bands, feedforward_norm_factor)
    hidden = entry_product(ffn_normed, ffn_own, ffn_one, ffn_two, ffn_far)
    units = hidden.shape[1] // 2
    active = (
        jax.nn.silu(hidden[:, :units] * half_of(switch_factors, side, 0))
        * (hidden[:, units:] * half_of(expand_factors, side, 0))
    ).astype(bf16)
    parts = result_bands(active, down_own, down_one, down_two, down_far, 1)
    results = []
    for k in range(2):
        reduced = tp_reduced(parts[k], parts[k + 2]).astype(bf16)
        total = reduced[:steps].astype(f32) + across_rep(reduced[steps:]).astype(f32)
        own_stream = stream[:steps, k * band : (k + 1) * band].astype(f32)
        results.append((own_stream + total).astype(bf16))
    return jnp.where(
        fs_index % 2 == 0,
        jnp.concatenate(results, axis=1),
        jnp.concatenate(results[::-1], axis=1),
    )


def on_device(*args):
    channels = args[2].shape[1]
    pairs = lax.axis_size("rep") % 2 == 0 and lax.axis_size("tp") == 2
    if pairs and lax.axis_size("fs") == 4 and channels % (2 * GROUP_DIM) == 0:
        return on_device_paired(*args)
    return on_device_gathered(*args)


def solution(mesh):
    return jax.shard_map(
        on_device,
        mesh=mesh,
        in_specs=(
            P(("rep", "fs"), None),
            P(),
            P("fs", "tp"),
            P("tp"),
            P("fs", "tp"),
            P("tp"),
            P("tp"),
            P(),
            P(),
            P("tp", "fs"),
            P("fs"),
            P(),
            P("fs", "tp"),
            P("tp"),
            P("fs", "tp"),
            P("tp"),
            P("tp", "fs"),
            P("fs"),
        ),
        out_specs=P(("rep", "fs"), "tp"),
        check_vma=False,
    )
```

```python
import jax
import jax.numpy as jnp
from jax import lax
from jax.sharding import PartitionSpec as P

BLENDER_FEATURES = 1024
GROUP_DIM = 128
BLOCK = 128


epsilon = 1e-06


def normalize(values, gain):
    return values * lax.rsqrt(jnp.mean(values * values, axis=-1, keepdims=True) + epsilon) * gain


def assembled_entries(pieces, activations):
    segments = (
        lax.all_gather(pieces[0], "fs", axis=0, tiled=True),
        lax.all_gather(pieces[1], "fs", axis=0, tiled=True),
    )
    return tuple(
        (jnp.dot(activations, segment, preferred_element_type=jnp.float32) for segment in segments)
    )


def collect_cols(shard_rows, activations, scales):
    return (
        jnp.dot(
            activations,
            lax.all_gather(shard_rows, "fs", axis=1, tiled=True),
            preferred_element_type=jnp.float32,
        )
        * scales
    )


def on_device_gathered(
    skip_stream_entry,
    sequence_blender_factor,
    product_projector,
    product_side_factors,
    placewise_projector,
    placewise_entry_factors,
    placewise_rescale_factor,
    place_cluster_operator,
    placewise_offset_vector,
    blender_result_projector,
    blender_result_factors,
    feedforward_norm_factor,
    switch_projector,
    switch_factors,
    expand_projector,
    expand_factors,
    contract_projector,
    contract_factors,
):
    device_sequence_steps = skip_stream_entry.shape[0]
    tp_index = lax.axis_index("tp")
    own_features = skip_stream_entry.shape[1] // lax.axis_size("tp")
    out_scales = (
        lax.all_gather(blender_result_factors, "fs", axis=0, tiled=True),
        lax.all_gather(contract_factors, "fs", axis=0, tiled=True),
    )
    standardized_stream = normalize(
        skip_stream_entry.astype(jnp.float32), sequence_blender_factor
    ).astype(jnp.bfloat16)
    product_plain, diffuse_plain = assembled_entries(
        (product_projector.astype(jnp.bfloat16), placewise_projector.astype(jnp.bfloat16)),
        standardized_stream,
    )
    product_portion = jax.nn.gelu(product_plain * product_side_factors)
    spread = jax.nn.gelu(diffuse_plain * placewise_entry_factors)
    feature_total = spread.shape[1]
    squares = lax.psum(jnp.sum(spread * spread, axis=1), "tp")
    factor = lax.rsqrt(squares / BLENDER_FEATURES + epsilon)
    spread_normed = (spread * factor[:, None] * placewise_rescale_factor).astype(jnp.bfloat16)
    group_span = min(feature_total, GROUP_DIM)
    group_count = max(1, feature_total // GROUP_DIM)
    first_group = tp_index * feature_total // GROUP_DIM
    causal = jnp.tril(jnp.ones((BLOCK, BLOCK), dtype=bool))
    local_weight = lax.dynamic_slice_in_dim(place_cluster_operator, first_group, group_count, 0)
    local_weight = jnp.where(causal[None], local_weight, jnp.zeros_like(local_weight))
    local_bias = lax.dynamic_slice_in_dim(placewise_offset_vector, first_group, group_count, 0)
    blocks = spread_normed.reshape(device_sequence_steps // BLOCK, BLOCK, group_count, group_span)
    blended_sequence = jnp.einsum(
        "gts,nsgc->ntgc", local_weight, blocks, preferred_element_type=jnp.float32
    )
    blended_sequence = blended_sequence + local_bias.T[None, :, :, None]
    switched_inner = (
        product_portion * blended_sequence.reshape(device_sequence_steps, feature_total)
    ).astype(jnp.bfloat16)
    mix_terms = collect_cols(
        blender_result_projector.astype(jnp.bfloat16), switched_inner, out_scales[0]
    )
    mix_total = lax.psum_scatter(
        mix_terms.astype(jnp.bfloat16), "tp", scatter_dimension=1, tiled=True
    ).astype(jnp.float32)
    own_input = lax.dynamic_slice_in_dim(
        skip_stream_entry, tp_index * own_features, own_features, 1
    )
    stream = (own_input.astype(jnp.float32) + mix_total).astype(jnp.bfloat16)
    stream_whole = lax.all_gather(stream, "tp", axis=1, tiled=True)
    ffn_normed = normalize(stream_whole.astype(jnp.float32), feedforward_norm_factor).astype(
        jnp.bfloat16
    )
    gate_raw, up_raw = assembled_entries(
        (switch_projector.astype(jnp.bfloat16), expand_projector.astype(jnp.bfloat16)), ffn_normed
    )
    active = (jax.nn.silu(gate_raw * switch_factors) * (up_raw * expand_factors)).astype(
        jnp.bfloat16
    )
    ffn_terms = collect_cols(contract_projector.astype(jnp.bfloat16), active, out_scales[1])
    ffn_total = lax.psum_scatter(
        ffn_terms.astype(jnp.bfloat16), "tp", scatter_dimension=1, tiled=True
    ).astype(jnp.float32)
    return (stream.astype(jnp.float32) + ffn_total).astype(jnp.bfloat16)


def half_of(array, index, axis):
    lower, upper = jnp.split(array, 2, axis=axis)
    return jnp.where(index == 0, lower, upper)


def swap_pairs(size, bit):
    return [(i, i ^ bit) for i in range(size)]


def gather_first(own):
    size = lax.axis_size("fs")
    return (
        lax.ppermute(own, "fs", swap_pairs(size, 1)),
        lax.ppermute(own, "fs", swap_pairs(size, 2)),
    )


def gather_second(from_one, from_two, axis):
    size = lax.axis_size("fs")
    lower = jnp.split(from_two, 2, axis=axis)[0]
    upper = jnp.split(from_one, 2, axis=axis)[1]
    return (
        lax.ppermute(lower, "fs", swap_pairs(size, 1)),
        lax.ppermute(upper, "fs", swap_pairs(size, 2)),
    )


def dot32(a, b):
    return jnp.dot(a, b, preferred_element_type=jnp.float32)


def entry_product(blocks, own, one, two, far):
    cut = far[0].shape[0]
    total = dot32(blocks[0], own) + dot32(blocks[1], one) + dot32(blocks[2], two)
    return total + dot32(blocks[3][:, :cut], far[0]) + dot32(blocks[3][:, cut:], far[1])


def on_device_paired(
    skip_stream_entry,
    sequence_blender_factor,
    product_projector,
    product_side_factors,
    placewise_projector,
    placewise_entry_factors,
    placewise_rescale_factor,
    place_cluster_operator,
    placewise_offset_vector,
    blender_result_projector,
    blender_result_factors,
    feedforward_norm_factor,
    switch_projector,
    switch_factors,
    expand_projector,
    expand_factors,
    contract_projector,
    contract_factors,
):
    bf16, f32 = jnp.bfloat16, jnp.float32
    steps, width = skip_stream_entry.shape
    rep_size, fs_size, tp_size = (lax.axis_size(a) for a in ("rep", "fs", "tp"))
    tp_index = lax.axis_index("tp")
    fs_index = lax.axis_index("fs")
    side = lax.axis_index("rep") % 2
    band = width // fs_size
    upper_band = fs_index // 2

    def across_tp(a):
        return lax.ppermute(a, "tp", swap_pairs(tp_size, 1))

    def across_rep(a):
        return lax.ppermute(a, "rep", swap_pairs(rep_size, 1))

    def across_both(a):
        pairs = [
            (r * tp_size + t, (r ^ 1) * tp_size + (t ^ 1))
            for r in range(rep_size)
            for t in range(tp_size)
        ]
        return lax.ppermute(a, ("rep", "tp"), pairs)

    def bands_of(array):
        return [
            lax.dynamic_slice_in_dim(array, (fs_index ^ k) * band, band, 1)
            for k in range(fs_size)
        ]

    def gains_of(gain):
        return [
            lax.dynamic_slice_in_dim(gain, (fs_index ^ k) * band, band, 0)
            for k in range(fs_size)
        ]

    sent = across_rep(half_of(skip_stream_entry, tp_index, 1))
    other = across_tp(sent)

    in_own = jnp.concatenate(
        [half_of(product_projector, side, 1), half_of(placewise_projector, side, 1)], axis=1
    ).astype(bf16)
    out_own = half_of(blender_result_projector, side, 0).astype(bf16)
    in_one, in_two = gather_first(in_own)
    out_one, out_two = gather_first(out_own)
    scales_own = jnp.stack([blender_result_factors, contract_factors])
    scales = [scales_own] + [
        lax.ppermute(scales_own, "fs", swap_pairs(fs_size, k)) for k in range(1, fs_size)
    ]
    in_far = gather_second(in_one, in_two, 0)
    out_far = gather_second(out_one, out_two, 1)
    ffn_own = jnp.concatenate(
        [half_of(switch_projector, side, 1), half_of(expand_projector, side, 1)], axis=1
    ).astype(bf16)
    down_own = half_of(contract_projector, side, 0).astype(bf16)
    ffn_one, ffn_two = gather_first(ffn_own)
    down_one, down_two = gather_first(down_own)
    ffn_far = gather_second(ffn_one, ffn_two, 0)
    down_far = gather_second(down_one, down_two, 1)

    partner_rows = jnp.where(
        tp_index == 0,
        jnp.concatenate([sent, other], axis=1),
        jnp.concatenate([other, sent], axis=1),
    )
    rows = jnp.concatenate([skip_stream_entry, partner_rows], axis=0)
    row_bands = bands_of(rows)

    def normed_bands(bands, gain):
        wide = [b.astype(f32) for b in bands]
        total = sum(jnp.sum(b * b, axis=-1, keepdims=True) for b in wide)
        factor = lax.rsqrt(total / width + epsilon)
        return [(b * factor * g).astype(bf16) for b, g in zip(wide, gains_of(gain))]

    normed = normed_bands(row_bands, sequence_blender_factor)
    entry = entry_product(normed, in_own, in_one, in_two, in_far)
    channels = entry.shape[1] // 2
    carrier = jax.nn.gelu(entry[:, :channels] * half_of(product_side_factors, side, 0))
    spread = jax.nn.gelu(entry[:, channels:] * half_of(placewise_entry_factors, side, 0))
    squares = jnp.sum(spread * spread, axis=1)
    turned = jnp.concatenate([squares[steps:], squares[:steps]])
    squares = (squares + across_tp(squares)) + (across_rep(turned) + across_both(turned))
    factor = lax.rsqrt(squares / BLENDER_FEATURES + epsilon)
    spread_normed = (
        spread * factor[:, None] * half_of(placewise_rescale_factor, side, 0)
    ).astype(bf16)
    group_count = channels // GROUP_DIM
    first_group = (tp_index * 2 + side) * group_count
    causal = jnp.tril(jnp.ones((BLOCK, BLOCK), dtype=bool))
    local_weight = lax.dynamic_slice_in_dim(place_cluster_operator, first_group, group_count, 0)
    local_weight = jnp.where(causal[None], local_weight, jnp.zeros_like(local_weight))
    local_bias = lax.dynamic_slice_in_dim(placewise_offset_vector, first_group, group_count, 0)
    blocks = spread_normed.reshape(2 * steps // BLOCK, BLOCK, group_count, GROUP_DIM)
    blended = jnp.einsum("gts,nsgc->ntgc", local_weight, blocks, preferred_element_type=f32)
    blended = blended + local_bias.T[None, :, :, None]
    gated = (carrier * blended.reshape(2 * steps, channels)).astype(bf16)

    def result_bands(act, own, one, two, far, which):
        pieces = (own, one, two, jnp.concatenate(far, axis=1))
        results = []
        for w, s in zip(pieces, scales):
            results.append((dot32(act, w) * s[which]).astype(bf16))
        return results

    keep_low = tp_index == upper_band

    def tp_reduced(low, high):
        mine = jnp.where(keep_low, low, high)
        theirs = jnp.where(keep_low, high, low)
        return mine.astype(f32) + across_tp(theirs).astype(f32)

    parts = result_bands(gated, out_own, out_one, out_two, out_far, 0)
    mixed = tp_reduced(
        jnp.concatenate(parts[:2], axis=1), jnp.concatenate(parts[2:], axis=1)
    ).astype(bf16)
    away = across_rep(jnp.concatenate([mixed[steps:], mixed[:steps]], axis=0))
    mixed_total = mixed.astype(f32) + away.astype(f32)
    low_rows = jnp.concatenate(row_bands[:2], axis=1)
    high_rows = jnp.concatenate(row_bands[2:], axis=1)
    stream = (jnp.where(keep_low, low_rows, high_rows).astype(f32) + mixed_total).astype(bf16)
    stream_other = across_tp(stream)
    low_stream = jnp.where(keep_low, stream, stream_other)
    high_stream = jnp.where(keep_low, stream_other, stream)
    stream_bands = [
        low_stream[:, :band],
        low_stream[:, band:],
        high_stream[:, :band],
        high_stream[:, band:],
    ]
    ffn_normed = normed_bands(stream_bands, feedforward_norm_factor)
    hidden = entry_product(ffn_normed, ffn_own, ffn_one, ffn_two, ffn_far)
    units = hidden.shape[1] // 2
    active = (
        jax.nn.silu(hidden[:, :units] * half_of(switch_factors, side, 0))
        * (hidden[:, units:] * half_of(expand_factors, side, 0))
    ).astype(bf16)
    parts = result_bands(active, down_own, down_one, down_two, down_far, 1)
    results = []
    for k in range(2):
        reduced = tp_reduced(parts[k], parts[k + 2]).astype(bf16)
        away = across_rep(reduced[steps:])
        total = reduced[:steps].astype(f32) + away.astype(f32)
        own_stream = stream[:steps, k * band : (k + 1) * band].astype(f32)
        results.append((own_stream + total).astype(bf16))
    return jnp.where(
        fs_index % 2 == 0,
        jnp.concatenate(results, axis=1),
        jnp.concatenate(results[::-1], axis=1),
    )


def on_device(*args):
    channels = args[2].shape[1]
    pairs = lax.axis_size("rep") % 2 == 0 and lax.axis_size("tp") == 2
    if pairs and lax.axis_size("fs") == 4 and channels % (2 * GROUP_DIM) == 0:
        return on_device_paired(*args)
    return on_device_gathered(*args)


def solution(mesh):
    return jax.shard_map(
        on_device,
        mesh=mesh,
        in_specs=(
            P(("rep", "fs"), None),
            P(),
            P("fs", "tp"),
            P("tp"),
            P("fs", "tp"),
            P("tp"),
            P("tp"),
            P(),
            P(),
            P("tp", "fs"),
            P("fs"),
            P(),
            P("fs", "tp"),
            P("tp"),
            P("fs", "tp"),
            P("tp"),
            P("tp", "fs"),
            P("fs"),
        ),
        out_specs=P(("rep", "fs"), "tp"),
        check_vma=False,
    )
```
